32 devices in a mesh: ep: 8 (over z, core), tp: 4 (over y, x).
Axes of the slice: x: 2, y: 2, z: 4, core: 2. Of those that a mesh axis runs over, the one named last changes fastest.
Arguments:
- queries: bfloat16 [2048, 4096], P('ep', 'tp'), may hold values from -6 to 6
- keys: bfloat16 [2048, 1024], P('ep', 'tp'), may hold values from -6 to 6
- values: bfloat16 [2048, 1024], P('ep', 'tp'), may hold values from -6 to 6
- query_gain: float32 [64], replicated, may hold values from 1 to 11
- key_gain: float32 [64], replicated, may hold values from 1 to 11
- moe_rows: bfloat16 [2048, 4096], P('ep', 'tp'), may hold values from -14 to 14
- route_ids: int32 [2048, 2], P('ep'), may hold values from 0 to 7, all different within a row; in each aligned block of 256 rows (0 to 255, 256 to 511, ...) at most 96 rows name the same one
- group_weight: float32 [2048], P('ep'), may hold values from 0.2 to 1
- expert_weight: float32 [2048, 2], P('ep'), may hold values from 0.05 to 1
- expert_gate: bfloat16 [8, 4096, 2048], P('ep', None, 'tp'), may hold values from -0.09375 to 0.09375
- expert_up: bfloat16 [8, 4096, 2048], P('ep', None, 'tp'), may hold values from -0.09375 to 0.09375
- expert_down: bfloat16 [8, 2048, 4096], P('ep', None, 'tp'), may hold values from -0.125 to 0.125
Outputs:
- attended: bfloat16 [2048, 4096], P('ep', 'tp')
- moe_out: bfloat16 [2048, 4096], P('ep', 'tp')
The draws below stay inside these ranges and needn't reach their ends.
Inputs may be any that keep to these rules, and one draw needn't show every extreme that they name: `route_ids`: each row names 2 different experts. Among the rows of one device no expert is named by more than 96 rows, and in every draw some expert is named by exactly 96 of them.
All inputs are finite; a program needn't handle non-finite values.
Results may differ from the reference program's by a relative error of at most 0.0055.
The reference program's roundings to bfloat16 on the way count: a program that leaves them out, or rounds other values in their place, can miss the bound.
Values may be sent and summed in bfloat16 or wider, within the bound.
A program may use at most 128 MiB of HBM per device.

```python
import math
import jax
import jax.numpy as jnp
import numpy as np
from jax import lax

D = 4096
HEAD_DIM = 64
HEADS = 64
KV_HEADS = 16
FF = 2048
GRID_W = 64
TOPK = 2
TOK_DEV = 256
TOKENS = 2048
EXPERTS = 8
CAP = 96
N_EP = 8


def query_key_pair(key):
    folded = jax.random.fold_in(key, 17)
    key_one, key_two = jax.random.split(folded, 2)
    query_draw = jnp.clip(jax.random.normal(key_one, (TOKENS, HEADS * HEAD_DIM), jnp.float32), -6.0, 6.0)
    key_draw = jnp.clip(jax.random.normal(key_two, (TOKENS, KV_HEADS * HEAD_DIM), jnp.float32), -6.0, 6.0)
    return (query_draw, key_draw)


def draw_queries(key, part):
    return query_key_pair(key)[0].astype(jnp.bfloat16)


def draw_keys(key, part):
    return query_key_pair(key)[1].astype(jnp.bfloat16)


def gain_draw(key, salt):
    folded = jax.random.fold_in(key, salt)
    spread = 1.5 * jnp.exp(jax.random.uniform(folded, (HEAD_DIM,), jnp.float32, -0.3, 0.3))
    return spread


def draw_query_gain(key, part):
    return gain_draw(key, 31)


def draw_key_gain(key, part):
    return gain_draw(key, 37)


def draw_moe_rows(key, part):
    folded = jax.random.fold_in(key, 23)
    key_one, key_two = jax.random.split(folded)
    base_part = jnp.clip(jax.random.normal(key_one, (TOKENS, D), jnp.float32), -4.0, 4.0)
    scales = jnp.exp(jax.random.uniform(key_two, (TOKENS, 1), jnp.float32, -1.2, 1.2))
    return (base_part * scales).astype(jnp.bfloat16)


def steps_of(rng, extent, cuts, least, top_value):
    factor_of = 1.0
    for dim, parts in cuts:
        heights = jax.random.uniform(jax.random.fold_in(jax.random.fold_in(rng, 6), dim), (parts,), jnp.float32, least / len(cuts), top_value / len(cuts))
        factor_of = factor_of * jnp.repeat(jnp.exp(heights), extent[dim] // parts).reshape((-1,) + (1,) * (len(extent) - 1 - dim))
    return factor_of


def assign_block(stream_key, own, number, rows, count, top, bound, slope):
    sequence = jax.random.permutation(stream_key, count)
    crowded, ordinary = load_shares(count, rows * top, bound, slope, True), load_shares(count, rows * top, bound, slope, False)
    places = jnp.arange(count)

    def named(lengths, offset_by):
        used = int((lengths > 0).sum())
        fixed = max(1, used // 4)
        moved = fixed + (places - fixed + offset_by * (used - fixed)) % max(1, count - fixed)
        return jnp.zeros((count,), jnp.int32).at[sequence[jnp.where(places < fixed, places, moved)]].set(jnp.asarray(lengths, jnp.int32))

    lengths = jnp.where(number % 4 == 0, named(crowded, number // 4), named(ordinary, number - number // 4 - 1))
    mixed = jax.random.permutation(jax.random.fold_in(own, 3), count)
    source_of, taker = mixed[0:count // 2 * 2:2], mixed[1:count // 2 * 2:2]
    margin = jnp.minimum(lengths[source_of] - 1, bound - lengths[taker]) // 2
    margin = jnp.where((source_of == sequence[0]) | (taker == sequence[0]) | (lengths[taker] == 0), 0, jnp.maximum(margin, 0))
    moved = jax.random.randint(jax.random.fold_in(own, 4), (count // 2,), 0, 1 << 20) % (margin + 1)
    lengths = lengths.at[source_of].add(-moved).at[taker].add(moved)
    labels = jnp.searchsorted(jnp.cumsum(lengths), jnp.arange(rows * top), side="right").astype(jnp.int32)
    table = labels.reshape(top, rows).T
    table = table[jax.random.permutation(jax.random.fold_in(own, 1), rows)]
    offset_by = jax.random.randint(jax.random.fold_in(own, 2), (rows, 1), 0, top)
    return jnp.take_along_axis(table, (jnp.arange(top)[None, :] + offset_by) % top, axis=1)


def load_shares(amount, total, bound, skew, full):
    portions = [(1 << 20) // math.isqrt(grade ** skew) + 1 for grade in range(1, amount + 1)]
    largest = bound if full else min(bound, max(-(-total // amount), total * portions[0] // sum(portions)))
    least = 1 if total - largest >= amount - 1 else 0
    counts, spare = [largest] + [least] * (amount - 1), total - largest - least * (amount - 1)
    while spare > 0:
        candidates = [i for i in range(1, amount) if counts[i] < largest] or [i for i in range(1, amount) if counts[i] < bound]
        whole, remaining = sum([portions[i] for i in candidates]), spare
        for i in candidates:
            addition = min(bound - counts[i], max(1, remaining * portions[i] // whole), spare)
            counts[i] = counts[i] + addition
            spare = spare - addition
    return np.array(counts)


def normal_values(own_key, dims, deviation, bound, cuts=(), kind=jnp.bfloat16):
    entries = deviation * jax.random.normal(own_key, dims, jnp.float32)
    if cuts:
        entries = entries * steps_of(own_key, dims, cuts, -0.22, 0.18)
    return jnp.clip(entries, -bound, bound).astype(kind)


def setup_inputs(seed: int = 0) -> dict:
    key_of = jax.random.split(jax.random.key(seed), 13)
    queries = draw_queries(jax.random.fold_in(key_of[12], 71), 0)
    keys = draw_keys(jax.random.fold_in(key_of[12], 71), 0)
    values = normal_values(key_of[2], (TOKENS, KV_HEADS * HEAD_DIM), 1.0, 6.0, ((0, 8), (1, 4)))
    query_gain = draw_query_gain(jax.random.fold_in(key_of[12], 71), 0)
    key_gain = draw_key_gain(jax.random.fold_in(key_of[12], 71), 0)
    moe_rows = draw_moe_rows(jax.random.fold_in(key_of[12], 71), 0)
    route_ids_keys = jax.random.split(jax.random.fold_in(key_of[6], 1), TOKENS // TOK_DEV)
    route_ids_turns = jax.random.permutation(jax.random.fold_in(key_of[6], 3), TOKENS // TOK_DEV)
    route_ids = jax.vmap(lambda own, number: assign_block(jax.random.fold_in(key_of[6], 2), own, number, TOK_DEV, EXPERTS, TOPK, CAP, 1))(route_ids_keys, route_ids_turns).reshape((TOKENS, TOPK))
    group_weight = jnp.clip(jnp.exp(math.log(1.0) - 1.609438 * jax.random.uniform(key_of[7], (TOKENS,), jnp.float32) ** steps_of(key_of[7], (TOKENS,), ((0, 8),), -0.2, 0.2)), 0.2, 1.0)
    expert_weight = jnp.clip(jnp.exp(math.log(1.0) - 2.9957323 * jax.random.uniform(key_of[8], (TOKENS, TOPK), jnp.float32) ** steps_of(key_of[8], (TOKENS, TOPK), ((0, 8),), -0.2, 0.2)), 0.05, 1.0)
    expert_gate = normal_values(key_of[9], (EXPERTS, D, FF), D ** -0.5, 0.09375, ((0, 8), (2, 4)))
    expert_up = normal_values(key_of[10], (EXPERTS, D, FF), D ** -0.5, 0.09375, ((0, 8), (2, 4)))
    expert_down = normal_values(key_of[11], (EXPERTS, FF, D), FF ** -0.5, 0.125, ((0, 8), (2, 4)))
    return dict(queries=queries, keys=keys, values=values, query_gain=query_gain, key_gain=key_gain, moe_rows=moe_rows, route_ids=route_ids, group_weight=group_weight, expert_weight=expert_weight, expert_gate=expert_gate, expert_up=expert_up, expert_down=expert_down)


def rotary_tables(position):
    pair_count = HEAD_DIM // 4
    grid_pos = jnp.stack([position // GRID_W, position % GRID_W], axis=-1).astype(jnp.float32)
    frequency = 10000.0 ** (-jnp.arange(pair_count, dtype=jnp.float32) / pair_count)
    angles = grid_pos[:, :, None] * frequency
    return (jnp.cos(angles), jnp.sin(angles))

def normed_rotated(rows_in, gain, cosine, sine_of):
    row_count, head_count = (rows_in.shape[0], rows_in.shape[1])
    pair_count = HEAD_DIM // 4
    scaled = rows_in * lax.rsqrt(lax.optimization_barrier(jnp.mean(rows_in * rows_in, axis=-1, keepdims=True)) + 1e-06) * gain
    parted = scaled.reshape(row_count, head_count, 2, 2, pair_count)
    first_half, second = (parted[:, :, :, 0, :], parted[:, :, :, 1, :])
    cos_b, sin_b = (cosine[:, None], sine_of[:, None])
    turned = jnp.stack([first_half * cos_b - second * sin_b, second * cos_b + first_half * sin_b], axis=3)
    return turned.reshape(row_count, head_count, HEAD_DIM).astype(jnp.bfloat16)

def attend_reference(queries, keys, values, query_gain, key_gain):
    group_size = HEADS // KV_HEADS
    cosine, sine_of = rotary_tables(jnp.arange(TOKENS, dtype=jnp.int32))
    query_rot = normed_rotated(queries.astype(jnp.float32).reshape(TOKENS, HEADS, HEAD_DIM), query_gain, cosine, sine_of)
    key_rot = normed_rotated(keys.astype(jnp.float32).reshape(TOKENS, KV_HEADS, HEAD_DIM), key_gain, cosine, sine_of)
    value_heads = values.reshape(TOKENS, KV_HEADS, HEAD_DIM)
    block_rows = math.gcd(TOKENS, 512)
    query_heads = query_rot.reshape(TOKENS // block_rows, block_rows, KV_HEADS, group_size, HEAD_DIM).transpose(2, 0, 1, 3, 4)

    def one_head(inputs):
        q_part, k_head, v_head = inputs

        def one_block(q_blk):
            scores = jnp.einsum('qgd,sd->gqs', q_blk.astype(jnp.float32), k_head.astype(jnp.float32)) * HEAD_DIM ** (-0.5)
            weights = jnp.exp(scores - lax.optimization_barrier(jnp.max(scores, axis=-1, keepdims=True)))
            denominator = lax.optimization_barrier(jnp.sum(weights, axis=-1))
            low_weights = lax.optimization_barrier(weights.astype(jnp.bfloat16)).astype(jnp.float32)
            mixed_out = jnp.einsum('gqs,sd->qgd', low_weights, v_head.astype(jnp.float32))
            return (mixed_out / denominator.T[:, :, None]).astype(jnp.bfloat16)
        return lax.map(one_block, q_part)
    output = lax.map(one_head, (query_heads, key_rot.transpose(1, 0, 2), value_heads.transpose(1, 0, 2)))
    return output.transpose(1, 2, 0, 3, 4).reshape(TOKENS, HEADS * HEAD_DIM)

def experts_reference(moe_rows, route_ids, group_weight, expert_weight, expert_gate, expert_up, expert_down):
    picks = TOK_DEV * TOPK
    route_list = route_ids.reshape(N_EP, picks)
    one_hot = (route_list[:, :, None] == jnp.arange(EXPERTS, dtype=jnp.int32)[None, None, :]).astype(jnp.int32)
    rank_of = lax.optimization_barrier(jnp.sum((jnp.cumsum(one_hot, axis=1) - one_hot) * one_hot, axis=-1))
    source = jnp.arange(N_EP, dtype=jnp.int32)[:, None]
    slot_of = route_list * (N_EP * CAP) + source * CAP + rank_of
    owner_of = source * TOK_DEV + jnp.arange(picks, dtype=jnp.int32)[None, :] // TOPK
    slot_owner = jnp.full((EXPERTS * N_EP * CAP,), TOKENS, jnp.int32).at[slot_of.reshape(-1)].set(owner_of.reshape(-1))
    padded = jnp.concatenate([moe_rows, jnp.zeros((1, D), moe_rows.dtype)], axis=0)
    routed = padded[slot_owner].reshape(EXPERTS, N_EP * CAP, D)

    def one_expert(inputs):
        rows_in, w_gate, w_up, w_down = inputs
        widened = rows_in.astype(jnp.float32)
        inv_rms = lax.rsqrt(lax.optimization_barrier(jnp.mean(widened * widened, axis=-1, keepdims=True)) + 1e-06)
        gate_act = jnp.dot(rows_in, w_gate, preferred_element_type=jnp.float32) * inv_rms
        up_act = jnp.dot(rows_in, w_up, preferred_element_type=jnp.float32) * inv_rms
        hidden = (jax.nn.silu(gate_act) * up_act).astype(jnp.bfloat16)
        return jnp.dot(hidden, w_down, preferred_element_type=jnp.float32).astype(jnp.bfloat16)
    results = lax.map(one_expert, (routed, expert_gate, expert_up, expert_down)).reshape(EXPERTS * N_EP * CAP, D)
    picked = results[slot_of.reshape(TOKENS, TOPK)].astype(jnp.float32)
    mixing = group_weight[:, None] * expert_weight / lax.optimization_barrier(jnp.sum(expert_weight, axis=-1, keepdims=True))
    return lax.optimization_barrier(jnp.sum(mixing[:, :, None] * picked, axis=1)).astype(jnp.bfloat16)

def reference(queries, keys, values, query_gain, key_gain, moe_rows, route_ids, group_weight, expert_weight, expert_gate, expert_up, expert_down):
    attended = attend_reference(queries, keys, values, query_gain, key_gain)
    moe_out = experts_reference(moe_rows, route_ids, group_weight, expert_weight, expert_gate, expert_up, expert_down)
    return (attended, moe_out)
```

```python
import jax
import jax.numpy as jnp
from jax import lax
from jax.sharding import PartitionSpec as P

D = 4096
HEAD_DIM = 64
GRID_W = 64
TOPK = 2
CHUNKS = 2


def rotary_tables(position):
    pair_count = HEAD_DIM // 4
    grid_pos = jnp.stack([position // GRID_W, position % GRID_W], axis=-1).astype(jnp.float32)
    frequency = 10000.0 ** (-jnp.arange(pair_count, dtype=jnp.float32) / pair_count)
    angles = grid_pos[:, :, None] * frequency
    return (jnp.cos(angles), jnp.sin(angles))


def normed_rotated(rows_in, gain, cosine, sine_of):
    row_count, head_count = (rows_in.shape[0], rows_in.shape[1])
    pair_count = HEAD_DIM // 4
    scaled = rows_in * lax.rsqrt(jnp.mean(rows_in * rows_in, axis=-1, keepdims=True) + 1e-06) * gain
    parted = scaled.reshape(row_count, head_count, 2, 2, pair_count)
    first_half, second = (parted[:, :, :, 0, :], parted[:, :, :, 1, :])
    cos_b, sin_b = (cosine[:, None], sine_of[:, None])
    turned = jnp.stack(
        [first_half * cos_b - second * sin_b, second * cos_b + first_half * sin_b], axis=3
    )
    return turned.reshape(row_count, head_count, HEAD_DIM).astype(jnp.bfloat16)


def attention(query_rot, portion, kv_width):
    key_count = portion.shape[0]
    head_count = kv_width // HEAD_DIM
    keys_part = portion[:, :kv_width].reshape(key_count, head_count, HEAD_DIM)
    values_part = portion[:, kv_width:].reshape(key_count, head_count, HEAD_DIM)
    scores = jnp.einsum(
        "tkgd,skd->kgts", query_rot, keys_part, preferred_element_type=jnp.float32
    ) * HEAD_DIM ** (-0.5)
    weights = jnp.exp(scores - jnp.max(scores, axis=-1, keepdims=True))
    denominator = jnp.sum(weights, axis=-1)
    summed = jnp.einsum(
        "kgts,skd->kgtd",
        weights.astype(jnp.bfloat16),
        values_part,
        preferred_element_type=jnp.float32,
    )
    return summed / denominator[..., None]


def on_device(
    queries,
    keys,
    values,
    query_gain,
    key_gain,
    moe_rows,
    route_ids,
    group_weight,
    expert_weight,
    expert_gate,
    expert_up,
    expert_down,
):
    ep = lax.axis_size("ep")
    tp = lax.axis_size("tp")
    me = lax.axis_index("ep")
    moe_tokens, chan = moe_rows.shape
    total = moe_tokens * ep
    capacity = 3 * moe_tokens * TOPK // (2 * ep) * ep
    everyone = lax.all_gather(moe_rows, "ep", axis=0, tiled=True)
    mixing = group_weight[:, None] * expert_weight / jnp.sum(expert_weight, axis=1, keepdims=True)
    table = lax.all_gather(
        jnp.concatenate([route_ids.astype(jnp.float32), mixing], axis=1).T, "ep", axis=1, tiled=True
    )
    mine = table[:TOPK] == me.astype(jnp.float32)
    chosen = jnp.any(mine, axis=0)
    mix_here = jnp.sum(jnp.where(mine, table[TOPK:], 0.0), axis=0)
    flags = chosen.reshape(ep, moe_tokens).astype(jnp.bfloat16)
    upper = jnp.triu(jnp.ones((moe_tokens, moe_tokens), jnp.bfloat16), 1)
    inner = jnp.dot(flags, upper, preferred_element_type=jnp.float32)
    counts = jnp.sum(flags.astype(jnp.float32), axis=1)
    earlier = jnp.sum(jnp.where(jnp.arange(ep)[None, :] < jnp.arange(ep)[:, None], counts[None, :], 0.0), axis=1)
    slot = (inner + earlier[:, None]).reshape(total).astype(jnp.int32)
    slot = jnp.where(chosen, slot, -1)

    tok_rows = queries.shape[0]
    q_heads = queries.shape[1] // HEAD_DIM
    k_heads = keys.shape[1] // HEAD_DIM
    group_size = q_heads // k_heads
    position = me * tok_rows + jnp.arange(tok_rows, dtype=jnp.int32)
    cosine, sine_of = rotary_tables(position)
    key_rot = normed_rotated(
        keys.astype(jnp.float32).reshape(tok_rows, k_heads, HEAD_DIM), key_gain, cosine, sine_of
    )
    kv_width = k_heads * HEAD_DIM
    joined = jnp.concatenate([key_rot.reshape(tok_rows, kv_width), values], axis=1)
    query_rot = normed_rotated(
        queries.astype(jnp.float32).reshape(tok_rows, q_heads, HEAD_DIM),
        query_gain,
        cosine,
        sine_of,
    )
    query_rot = query_rot.reshape(tok_rows, k_heads, group_size, HEAD_DIM)

    rows = capacity // CHUNKS
    gate_w = expert_gate[0].reshape(tp, chan, -1)
    up_w = expert_up[0].reshape(tp, chan, -1)
    down_w = expert_down[0].reshape(tp, -1, expert_down.shape[2])
    picks = []
    for c in range(CHUNKS):
        one_hot = (
            slot[None, :] == (c * rows + jnp.arange(rows, dtype=jnp.int32))[:, None]
        ).astype(jnp.bfloat16)
        picks.append(
            jnp.dot(one_hot, everyone, preferred_element_type=jnp.float32).astype(jnp.bfloat16)
        )
    gathered = [lax.all_gather(picks[0], "tp", axis=0)]
    kv_all = lax.all_gather(joined, "ep", axis=0, tiled=True)
    for c in range(1, CHUNKS):
        gathered.append(lax.all_gather(picks[c], "tp", axis=0))
    results = []
    for c in range(CHUNKS):
        portion = gathered[c]
        widened = portion.astype(jnp.float32)
        square_sum = jnp.sum(widened * widened, axis=(0, 2))
        inv_rms = lax.rsqrt(square_sum / D + 1e-06)[:, None]
        gate_act = jnp.einsum("ard,adf->rf", portion, gate_w, preferred_element_type=jnp.float32)
        up_act = jnp.einsum("ard,adf->rf", portion, up_w, preferred_element_type=jnp.float32)
        hidden = (jax.nn.silu(gate_act * inv_rms) * (up_act * inv_rms)).astype(jnp.bfloat16)
        hidden_all = lax.all_gather(hidden, "tp", axis=0)
        results.append(
            jnp.einsum(
                "arf,afd->rd", hidden_all, down_w, preferred_element_type=jnp.float32
            ).astype(jnp.bfloat16)
        )
    result = jnp.concatenate(results, axis=0)
    back = (slot[:, None] == jnp.arange(capacity, dtype=jnp.int32)[None, :]).astype(jnp.bfloat16)
    spread = (
        jnp.dot(back, result, preferred_element_type=jnp.float32) * mix_here[:, None]
    ).astype(jnp.bfloat16)
    moe_out = lax.psum_scatter(spread, "ep", scatter_dimension=0, tiled=True)

    attended = (
        attention(query_rot, kv_all, kv_width)
        .transpose(2, 0, 1, 3)
        .reshape(tok_rows, q_heads * HEAD_DIM)
        .astype(jnp.bfloat16)
    )
    return (attended, moe_out)


def solution(mesh):
    placed = (
        P("ep", "tp"),
        P("ep", "tp"),
        P("ep", "tp"),
        P(),
        P(),
        P("ep", "tp"),
        P("ep", None),
        P("ep"),
        P("ep", None),
        P("ep", None, "tp"),
        P("ep", None, "tp"),
        P("ep", None, "tp"),
    )
    return jax.shard_map(
        on_device,
        mesh=mesh,
        in_specs=placed,
        out_specs=(P("ep", "tp"), P("ep", "tp")),
        check_vma=False,
    )
```

```python
import jax
import jax.numpy as jnp
from jax import lax
from jax.experimental import pallas as pl
from jax.experimental.pallas import tpu as pltpu
from jax.sharding import PartitionSpec as P

D = 4096
HEAD_DIM = 64
GRID_W = 64
TOPK = 2


def rotary_tables(position):
    pair_count = HEAD_DIM // 4
    grid_pos = jnp.stack([position // GRID_W, position % GRID_W], axis=-1).astype(jnp.float32)
    frequency = 10000.0 ** (-jnp.arange(pair_count, dtype=jnp.float32) / pair_count)
    angles = grid_pos[:, :, None] * frequency
    return (jnp.cos(angles), jnp.sin(angles))


def normed_rotated(rows_in, gain, cosine, sine_of):
    row_count, head_count = (rows_in.shape[0], rows_in.shape[1])
    pair_count = HEAD_DIM // 4
    scaled = rows_in * lax.rsqrt(jnp.mean(rows_in * rows_in, axis=-1, keepdims=True) + 1e-06) * gain
    parted = scaled.reshape(row_count, head_count, 2, 2, pair_count)
    first_half, second = (parted[:, :, :, 0, :], parted[:, :, :, 1, :])
    cos_b, sin_b = (cosine[:, None], sine_of[:, None])
    turned = jnp.stack(
        [first_half * cos_b - second * sin_b, second * cos_b + first_half * sin_b], axis=3
    )
    return turned.reshape(row_count, head_count, HEAD_DIM).astype(jnp.bfloat16)


def attend_block(carried, portion, query_rot, kv_width):
    running_max, denominator, summed = carried
    key_count = portion.shape[0]
    head_count = kv_width // HEAD_DIM
    keys_part = portion[:, :kv_width].reshape(key_count, head_count, HEAD_DIM)
    values_part = portion[:, kv_width:].reshape(key_count, head_count, HEAD_DIM)
    scores = jnp.einsum(
        "tkgd,skd->kgts", query_rot, keys_part, preferred_element_type=jnp.float32
    ) * HEAD_DIM ** (-0.5)
    new_max = jnp.max(scores, axis=-1)
    factor = jnp.exp(running_max - new_max)
    weights = jnp.exp(scores - new_max[..., None])
    denominator = denominator * factor + jnp.sum(weights, axis=-1)
    summed = summed * factor[..., None] + jnp.einsum(
        "kgts,skd->kgtd",
        weights.astype(jnp.bfloat16),
        values_part,
        preferred_element_type=jnp.float32,
    )
    return (new_max, denominator, summed)


def plain_on_device(
    queries,
    keys,
    values,
    query_gain,
    key_gain,
    moe_rows,
    route_ids,
    group_weight,
    expert_weight,
    expert_gate,
    expert_up,
    expert_down,
):
    tok_rows = queries.shape[0]
    q_heads = queries.shape[1] // HEAD_DIM
    k_heads = keys.shape[1] // HEAD_DIM
    group_size = q_heads // k_heads
    position = lax.axis_index("ep") * tok_rows + jnp.arange(tok_rows, dtype=jnp.int32)
    cosine, sine_of = rotary_tables(position)
    query_rot = normed_rotated(
        queries.astype(jnp.float32).reshape(tok_rows, q_heads, HEAD_DIM),
        query_gain,
        cosine,
        sine_of,
    )
    query_rot = query_rot.reshape(tok_rows, k_heads, group_size, HEAD_DIM)
    key_rot = normed_rotated(
        keys.astype(jnp.float32).reshape(tok_rows, k_heads, HEAD_DIM), key_gain, cosine, sine_of
    )
    kv_width = k_heads * HEAD_DIM
    joined = jnp.concatenate([key_rot.reshape(tok_rows, kv_width), values], axis=1)
    initial = (
        jnp.full((k_heads, group_size, tok_rows), -jnp.inf, jnp.float32),
        jnp.zeros((k_heads, group_size, tok_rows), jnp.float32),
        jnp.zeros((k_heads, group_size, tok_rows, HEAD_DIM), jnp.float32),
    )
    final_max, denominator, summed = attend_block(
        initial, lax.all_gather(joined, "ep", axis=0, tiled=True), query_rot, kv_width
    )
    attended = (
        (summed / denominator[..., None])
        .transpose(2, 0, 1, 3)
        .reshape(tok_rows, q_heads * HEAD_DIM)
        .astype(jnp.bfloat16)
    )
    moe_tokens = moe_rows.shape[0]
    local_experts = expert_gate.shape[0]
    expert_count = local_experts * lax.axis_size("ep")
    capacity = 3 * moe_tokens * TOPK // (2 * expert_count)
    picks = moe_tokens * TOPK
    route_list = route_ids.reshape(picks)
    one_hot = (route_list[:, None] == jnp.arange(expert_count, dtype=jnp.int32)[None, :]).astype(
        jnp.int32
    )
    rank_of = jnp.sum((jnp.cumsum(one_hot, axis=0) - one_hot) * one_hot, axis=1)
    slot_of = route_list * capacity + rank_of
    owner_of = (
        jnp.full((expert_count * capacity,), moe_tokens, jnp.int32)
        .at[slot_of]
        .set(jnp.arange(picks, dtype=jnp.int32) // TOPK)
    )
    padded = jnp.concatenate([moe_rows, jnp.zeros((1, moe_rows.shape[1]), moe_rows.dtype)], axis=0)
    arrived = lax.all_to_all(
        padded[owner_of].reshape(expert_count, capacity, moe_rows.shape[1]),
        "ep",
        split_axis=0,
        concat_axis=1,
        tiled=True,
    )
    portion = lax.all_gather(arrived, "tp", axis=2, tiled=True)
    widened = portion.astype(jnp.float32)
    gate_act = jnp.einsum("erd,edf->erf", portion, expert_gate, preferred_element_type=jnp.float32)
    up_act = jnp.einsum("erd,edf->erf", portion, expert_up, preferred_element_type=jnp.float32)
    square_sum = jnp.sum(widened * widened, axis=2)
    inv_rms = lax.rsqrt(square_sum / D + 1e-06)[..., None]
    hidden = (jax.nn.silu(gate_act * inv_rms) * (up_act * inv_rms)).astype(jnp.bfloat16)
    out_cols = expert_down.shape[2]
    expert_result = jnp.einsum(
        "erf,efd->erd",
        lax.all_gather(hidden, "tp", axis=2, tiled=True),
        expert_down,
        preferred_element_type=jnp.float32,
    ).astype(jnp.bfloat16)
    returned = lax.all_to_all(expert_result, "ep", split_axis=1, concat_axis=0, tiled=True)
    flat_back = returned.reshape(expert_count * capacity, out_cols)
    picked = flat_back[slot_of].reshape(moe_tokens, TOPK, out_cols).astype(jnp.float32)
    mixing = group_weight[:, None] * expert_weight / jnp.sum(expert_weight, axis=1, keepdims=True)
    moe_out = jnp.sum(mixing[:, :, None] * picked, axis=1).astype(jnp.bfloat16)
    return (attended, moe_out)


MESH = pl.DeviceIdType.MESH


def flip(index, mask, width):
    out = 0
    bit = 1
    while bit < width:
        a, b = (index // bit) % 2, (mask // bit) % 2
        out = out + bit * (a + b - 2 * a * b)
        bit *= 2
    return out


def rope_kernel(q_ref, k_ref, v_ref, qg_ref, kg_ref, cos_ref, sin_ref, qo_ref, kv_ref):
    rows = q_ref.shape[0]
    lane = lax.broadcasted_iota(jnp.int32, (rows, 128), 1)
    one = lax.broadcasted_iota(jnp.int32, (128, 128), 0) // HEAD_DIM
    two = lax.broadcasted_iota(jnp.int32, (128, 128), 1) // HEAD_DIM
    spread = jnp.where(one == two, 1.0 / HEAD_DIM, 0.0).astype(jnp.float32)
    first = lane % 32 < 16
    low = lane < HEAD_DIM
    cosine, sine_of = cos_ref[...], sin_ref[...]

    def turned(x, gain):
        x = x.astype(jnp.float32)
        mean = jnp.dot(
            x * x, spread, preferred_element_type=jnp.float32, precision=lax.Precision.HIGHEST
        )
        y = x * lax.rsqrt(mean + 1e-06) * gain
        partner = jnp.where(first, pltpu.roll(y, 112, 1), pltpu.roll(y, 16, 1))
        return y * cosine + partner * sine_of

    q_slabs = q_ref.shape[1] // 128
    k_slabs = k_ref.shape[1] // 128
    per_kv = q_slabs // (2 * k_slabs)
    for s in range(q_slabs):
        r = turned(q_ref[:, s * 128 : (s + 1) * 128], qg_ref[...])
        r = r.astype(jnp.bfloat16).astype(jnp.float32) * HEAD_DIM ** (-0.5)
        moved = pltpu.roll(r, HEAD_DIM, 1)
        if (s // per_kv) % 2 == 0:
            pair = (jnp.where(low, r, 0.0), jnp.where(low, moved, 0.0))
        else:
            pair = (jnp.where(low, 0.0, moved), jnp.where(low, 0.0, r))
        qo_ref[2 * s] = pair[0].astype(jnp.bfloat16)
        qo_ref[2 * s + 1] = pair[1].astype(jnp.bfloat16)
    for s in range(k_slabs):
        kv_ref[s] = turned(k_ref[:, s * 128 : (s + 1) * 128], kg_ref[...]).astype(jnp.bfloat16)
        kv_ref[k_slabs + s] = v_ref[:, s * 128 : (s + 1) * 128]


def main_kernel(
    ep, picks, kv, q_ref, s0_ref, s1_ref, mix_ref, wg_hbm, wu_hbm, wd_hbm,
    att_ref, moe_ref,
    xg, hid, res, ret, kvall, wg, wu, wd,
    w_sem, d_send, d_recv, x_send, x_recv, xr_send, xr_recv,
    h_send, h_recv, hr_send, hr_recv, r_send, r_recv, k_send, k_recv,
):
    me, tme = lax.axis_index("ep"), lax.axis_index("tp")
    tx, ty = flip(tme, 1, 4), flip(tme, 2, 4)
    sides = (tx, ty)
    cap = picks.shape[1]
    half = cap // 2
    pairs = ep // 2
    width = wg.shape[1]
    chan = picks.shape[2]

    weights = [
        pltpu.make_async_copy(a, b, w_sem.at[n])
        for n, (a, b) in enumerate(((wg_hbm.at[0], wg), (wu_hbm.at[0], wu), (wd_hbm.at[0], wd)))
    ]
    for copy in weights:
        copy.start()
    barrier = pltpu.get_barrier_semaphore()
    for j in range(1, ep):
        pl.semaphore_signal(barrier, inc=1, device_id={"ep": flip(me, j, ep)}, device_id_type=MESH)
    for side in sides:
        pl.semaphore_signal(barrier, inc=1, device_id={"tp": side}, device_id_type=MESH)
    pl.semaphore_wait(barrier, ep + 1)

    def remote(src, dst, send, recv, device):
        return pltpu.make_async_remote_copy(
            src_ref=src, dst_ref=dst, send_sem=send, recv_sem=recv,
            device_id=device, device_id_type=MESH,
        )

    def dispatch(j):
        to = flip(me, j, ep)
        return remote(picks.at[to], xg.at[j, tme], d_send.at[j], d_recv.at[j], {"ep": to})

    def keys_out(j):
        return remote(kv, kvall.at[me], k_send.at[j], k_recv.at[j], {"ep": flip(me, j, ep)})

    def keys_on(j):
        block = flip(me, j - 1, ep)
        return remote(
            kvall.at[block], kvall.at[block], k_send.at[j], k_recv.at[j], {"ep": flip(me, 1, ep)}
        )

    def cross(c, n, src=None):
        src = xg.at[c, tme] if src is None else src
        return remote(src, xg.at[c, tme], x_send.at[c, n], x_recv.at[c, n], {"tp": sides[n]})

    def cross_on(c, n):
        part = xg.at[c, sides[n], pl.ds(n * half, half)]
        return remote(part, part, xr_send.at[c, n], xr_recv.at[c, n], {"tp": sides[1 - n]})

    def wide(i, n):
        return remote(
            hid.at[i, tme], hid.at[i, tme], h_send.at[i, n], h_recv.at[i, n], {"tp": sides[n]}
        )

    def wide_on(i, n):
        part = hid.at[i, sides[n], pl.ds(n * cap, cap)]
        return remote(part, part, hr_send.at[i, n], hr_recv.at[i, n], {"tp": sides[1 - n]})

    def back(i, n):
        c = 2 * i + n
        return remote(
            res.at[i, pl.ds(n * cap, cap)], ret.at[me], r_send.at[c], r_recv.at[c],
            {"ep": flip(me, c, ep)},
        )

    for j in range(1, 4):
        dispatch(j).start()
    for j in range(1, ep):
        if j == 1 or j % 2 == 0:
            keys_out(j).start()
    for j in range(4, ep):
        dispatch(j).start()

    xg[0, tme] = picks[me]
    kvall[me] = kv[...]
    for n in range(2):
        cross(0, n, picks.at[me]).start()

    def enter(c):
        dispatch(c).wait_recv()
        for n in range(2):
            cross(c, n).start()

    def relay(i):
        for d in range(2):
            for n in range(2):
                cross(2 * i + d, n).wait_recv()
                cross_on(2 * i + d, n).start()

    for c in range(1, 4):
        enter(c)
    relay(0)
    for copy in weights:
        copy.wait()

    def first_half(i):
        for d in range(2):
            for n in range(2):
                cross_on(2 * i + d, n).wait_recv()
        gate = jnp.zeros((2 * cap, width), jnp.float32)
        up = jnp.zeros((2 * cap, width), jnp.float32)
        square = jnp.zeros((2 * cap, 1), jnp.float32)
        for a in range(4):
            x = xg[pl.ds(2 * i, 2), a].reshape(2 * cap, chan)
            w = x.astype(jnp.float32)
            square = square + jnp.sum(w * w, axis=1, keepdims=True)
            gate = gate + jnp.dot(
                x, wg[a * chan : (a + 1) * chan, :], preferred_element_type=jnp.float32
            )
            up = up + jnp.dot(
                x, wu[a * chan : (a + 1) * chan, :], preferred_element_type=jnp.float32
            )
        inv = lax.rsqrt(square / D + 1e-06)
        g = gate * inv
        hid[i, tme] = (g / (1.0 + jnp.exp(-g)) * (up * inv)).astype(jnp.bfloat16)
        for n in range(2):
            wide(i, n).start()

    def second_half(i):
        for n in range(2):
            wide_on(i, n).wait_recv()
        total = jnp.zeros((2 * cap, chan), jnp.float32)
        for a in range(4):
            total = total + jnp.dot(
                hid[i, a], wd[a * width : (a + 1) * width, :], preferred_element_type=jnp.float32
            )
        res[i] = total.astype(jnp.bfloat16)

        @pl.when(i > 0)
        def _():
            back(i, 0).start()

        @pl.when(i == 0)
        def _():
            ret[me] = res[0, :cap]

        back(i, 1).start()

    heads = q_ref.shape[0]
    slabs = heads // 2
    k_slabs = kv.shape[0] // 2
    per_kv = slabs // (2 * k_slabs)
    keys_total = ep * kv.shape[1]

    def attend(m, carry):
        pp = m // (2 * per_kv)
        k = kvall[:, pp].reshape(keys_total, 128)
        v = kvall[:, k_slabs + pp].reshape(keys_total, 128)
        outs = []
        for d in range(2):
            s = lax.dot_general(
                q_ref[2 * m + d], k, (((1,), (1,)), ((), ())), preferred_element_type=jnp.float32
            )
            p = jnp.exp(s - jnp.max(s, axis=1, keepdims=True))
            den = jnp.sum(p, axis=1, keepdims=True)
            o = jnp.dot(p.astype(jnp.bfloat16), v, preferred_element_type=jnp.float32)
            outs.append(o / den)
        low = lax.broadcasted_iota(jnp.int32, outs[0].shape, 1) < HEAD_DIM
        even = jnp.where(low, outs[0], pltpu.roll(outs[1], HEAD_DIM, 1))
        odd = jnp.where(low, pltpu.roll(outs[0], HEAD_DIM, 1), outs[1])
        side = ((m // per_kv) % 2).astype(jnp.float32)
        both = jnp.where(side == 0.0, even, odd)
        att_ref[:, pl.ds(pl.multiple_of(m * 128, 128), 128)] = both.astype(jnp.bfloat16)
        return carry

    def keys_relay():
        for j in range(2, ep, 2):
            keys_out(j).wait_recv()
            keys_on(j + 1).start()

    def keys_ready():
        keys_out(1).wait_recv()
        for j in range(2, ep, 2):
            keys_on(j + 1).wait_recv()

    def step(i, carry):
        first_half(i)

        @pl.when(i < pairs - 1)
        def _():
            relay(i + 1)

        @pl.when(i == 0)
        def _():
            keys_relay()

        @pl.when(i == 1)
        def _():
            keys_ready()

        @pl.when(i < pairs - 2)
        def _():
            enter(2 * i + 4)
            enter(2 * i + 5)

        begin = slabs * jnp.maximum(i - 1, 0) * 2 // 5
        begin = jnp.where(i == pairs - 1, slabs - 1, begin)
        end = jnp.where(i == 0, 0, slabs * i * 2 // 5)
        end = jnp.where(i == pairs - 2, slabs - 1, end)
        end = jnp.where(i == pairs - 1, slabs, end)
        lax.fori_loop(begin, end, attend, 0)
        for n in range(2):
            wide(i, n).wait_recv()
            wide_on(i, n).start()
        second_half(i)
        return carry

    lax.fori_loop(0, pairs, step, 0)

    for c in range(1, ep):
        back(c // 2, c % 2).wait_recv()
    everything = ret[...].reshape(ep * cap, chan)
    mix = mix_ref[...]
    one = jnp.dot(s0_ref[...], everything, preferred_element_type=jnp.float32)
    two = jnp.dot(s1_ref[...], everything, preferred_element_type=jnp.float32)
    moe_ref[...] = (mix[:, 0:1] * one + mix[:, 1:2] * two).astype(jnp.bfloat16)

    for c in range(ep):
        for n in range(2):
            cross(c, n).wait_send()
            cross_on(c, n).wait_send()
        if c > 0:
            dispatch(c).wait_send()
            back(c // 2, c % 2).wait_send()
            keys_out(c).wait_send()
    for i in range(pairs):
        for n in range(2):
            wide(i, n).wait_send()
            wide_on(i, n).wait_send()


def on_device(
    queries, keys, values, query_gain, key_gain, moe_rows, route_ids, group_weight,
    expert_weight, expert_gate, expert_up, expert_down,
):
    ep, tp = lax.axis_size("ep"), lax.axis_size("tp")
    moe_tokens, chan = moe_rows.shape
    cap = 3 * moe_tokens * TOPK // (2 * expert_gate.shape[0] * ep)
    fits = tp == 4 and ep == 8 and cap % 32 == 0 and expert_gate.shape[0] == 1
    if not fits or queries.shape[1] // 128 != 8 or keys.shape[1] // 128 != 2:
        return plain_on_device(
            queries, keys, values, query_gain, key_gain, moe_rows, route_ids, group_weight,
            expert_weight, expert_gate, expert_up, expert_down,
        )
    tok = queries.shape[0]
    position = lax.axis_index("ep") * tok + jnp.arange(tok, dtype=jnp.int32)
    lane = jnp.arange(128, dtype=jnp.int32)
    pair_count = HEAD_DIM // 4
    frequency = 10000.0 ** (-(lane % pair_count).astype(jnp.float32) / pair_count)
    on_rows = (lane // (2 * pair_count)) % 2 == 0
    grid_pos = jnp.where(
        on_rows[None, :], (position // GRID_W)[:, None], (position % GRID_W)[:, None]
    ).astype(jnp.float32)
    angles = grid_pos * frequency[None, :]
    sign = jnp.where((lane // pair_count) % 2 == 0, -1.0, 1.0).astype(jnp.float32)
    heads = queries.shape[1] // HEAD_DIM
    slabs = keys.shape[1] // 128
    q_turned, kv = pl.pallas_call(
        rope_kernel,
        out_shape=(
            jax.ShapeDtypeStruct((heads, tok, 128), jnp.bfloat16),
            jax.ShapeDtypeStruct((2 * slabs, tok, 128), jnp.bfloat16),
        ),
    )(
        queries, keys, values,
        jnp.tile(query_gain, 2)[None, :], jnp.tile(key_gain, 2)[None, :],
        jnp.cos(angles), jnp.sin(angles) * sign[None, :],
    )
    picks_all = moe_tokens * TOPK
    route_list = route_ids.reshape(picks_all)
    one_hot = (route_list[:, None] == jnp.arange(ep, dtype=jnp.int32)[None, :]).astype(jnp.int32)
    rank_of = jnp.sum((jnp.cumsum(one_hot, axis=0) - one_hot) * one_hot, axis=1)
    slot_of = (route_list * cap + rank_of).reshape(moe_tokens, TOPK)
    columns = jnp.arange(ep * cap, dtype=jnp.int32)[None, :]
    picked = [(slot_of[:, n : n + 1] == columns).astype(jnp.bfloat16) for n in range(TOPK)]
    sent = lax.dot_general(
        picked[0] + picked[1], moe_rows, (((0,), (0,)), ((), ())),
        preferred_element_type=jnp.float32,
    ).astype(jnp.bfloat16).reshape(ep, cap, chan)
    mixing = group_weight[:, None] * expert_weight / jnp.sum(expert_weight, axis=1, keepdims=True)
    width = expert_gate.shape[2]
    vmem = pl.BlockSpec(memory_space=pltpu.VMEM)
    hbm = pl.BlockSpec(memory_space=pl.ANY)
    dma = pltpu.SemaphoreType.DMA
    bf = jnp.bfloat16
    attended, moe_out = pl.pallas_call(
        lambda *refs: main_kernel(ep, *refs),
        out_shape=(
            jax.ShapeDtypeStruct(queries.shape, bf),
            jax.ShapeDtypeStruct(moe_rows.shape, bf),
        ),
        in_specs=[vmem] * 6 + [hbm] * 3,
        out_specs=(vmem, vmem),
        scratch_shapes=[
            pltpu.VMEM((ep, tp, cap, chan), bf),
            pltpu.VMEM((ep // 2, tp, 2 * cap, width), bf),
            pltpu.VMEM((ep // 2, 2 * cap, chan), bf),
            pltpu.VMEM((ep, cap, chan), bf),
            pltpu.VMEM((ep, 2 * slabs, tok, 128), bf),
            pltpu.VMEM(expert_gate.shape[1:], bf),
            pltpu.VMEM(expert_up.shape[1:], bf),
            pltpu.VMEM(expert_down.shape[1:], bf),
            dma((3,)), dma((ep,)), dma((ep,)),
            dma((ep, 2)), dma((ep, 2)), dma((ep, 2)), dma((ep, 2)),
            dma((ep // 2, 2)), dma((ep // 2, 2)), dma((ep // 2, 2)), dma((ep // 2, 2)),
            dma((ep,)), dma((ep,)), dma((ep,)), dma((ep,)),
        ],
        compiler_params=pltpu.CompilerParams(
            collective_id=0, has_side_effects=True, vmem_limit_bytes=60 * 1024 * 1024
        ),
    )(sent, kv, q_turned, picked[0], picked[1], mixing, expert_gate, expert_up, expert_down)
    return (attended, moe_out)


def solution(mesh):
    placed = (
        P("ep", "tp"),
        P("ep", "tp"),
        P("ep", "tp"),
        P(),
        P(),
        P("ep", "tp"),
        P("ep", None),
        P("ep"),
        P("ep", None),
        P("ep", None, "tp"),
        P("ep", None, "tp"),
        P("ep", None, "tp"),
    )
    return jax.shard_map(
        on_device,
        mesh=mesh,
        in_specs=placed,
        out_specs=(P("ep", "tp"), P("ep", "tp")),
        check_vma=False,
    )
```

```python
import jax
import jax.numpy as jnp
from jax import lax
from jax.experimental import pallas as pl
from jax.experimental.pallas import tpu as pltpu
from jax.sharding import PartitionSpec as P

D = 4096
HEAD_DIM = 64
GRID_W = 64
TOPK = 2


def rotary_tables(position):
    pair_count = HEAD_DIM // 4
    grid_pos = jnp.stack([position // GRID_W, position % GRID_W], axis=-1).astype(jnp.float32)
    frequency = 10000.0 ** (-jnp.arange(pair_count, dtype=jnp.float32) / pair_count)
    angles = grid_pos[:, :, None] * frequency
    return (jnp.cos(angles), jnp.sin(angles))


def normed_rotated(rows_in, gain, cosine, sine_of):
    row_count, head_count = (rows_in.shape[0], rows_in.shape[1])
    pair_count = HEAD_DIM // 4
    scaled = rows_in * lax.rsqrt(jnp.mean(rows_in * rows_in, axis=-1, keepdims=True) + 1e-06) * gain
    parted = scaled.reshape(row_count, head_count, 2, 2, pair_count)
    first_half, second = (parted[:, :, :, 0, :], parted[:, :, :, 1, :])
    cos_b, sin_b = (cosine[:, None], sine_of[:, None])
    turned = jnp.stack(
        [first_half * cos_b - second * sin_b, second * cos_b + first_half * sin_b], axis=3
    )
    return turned.reshape(row_count, head_count, HEAD_DIM).astype(jnp.bfloat16)


def attend_block(carried, portion, query_rot, kv_width):
    running_max, denominator, summed = carried
    key_count = portion.shape[0]
    head_count = kv_width // HEAD_DIM
    keys_part = portion[:, :kv_width].reshape(key_count, head_count, HEAD_DIM)
    values_part = portion[:, kv_width:].reshape(key_count, head_count, HEAD_DIM)
    scores = jnp.einsum(
        "tkgd,skd->kgts", query_rot, keys_part, preferred_element_type=jnp.float32
    ) * HEAD_DIM ** (-0.5)
    new_max = jnp.max(scores, axis=-1)
    factor = jnp.exp(running_max - new_max)
    weights = jnp.exp(scores - new_max[..., None])
    denominator = denominator * factor + jnp.sum(weights, axis=-1)
    summed = summed * factor[..., None] + jnp.einsum(
        "kgts,skd->kgtd",
        weights.astype(jnp.bfloat16),
        values_part,
        preferred_element_type=jnp.float32,
    )
    return (new_max, denominator, summed)


def plain_on_device(
    queries,
    keys,
    values,
    query_gain,
    key_gain,
    moe_rows,
    route_ids,
    group_weight,
    expert_weight,
    expert_gate,
    expert_up,
    expert_down,
):
    tok_rows = queries.shape[0]
    q_heads = queries.shape[1] // HEAD_DIM
    k_heads = keys.shape[1] // HEAD_DIM
    group_size = q_heads // k_heads
    position = lax.axis_index("ep") * tok_rows + jnp.arange(tok_rows, dtype=jnp.int32)
    cosine, sine_of = rotary_tables(position)
    query_rot = normed_rotated(
        queries.astype(jnp.float32).reshape(tok_rows, q_heads, HEAD_DIM),
        query_gain,
        cosine,
        sine_of,
    )
    query_rot = query_rot.reshape(tok_rows, k_heads, group_size, HEAD_DIM)
    key_rot = normed_rotated(
        keys.astype(jnp.float32).reshape(tok_rows, k_heads, HEAD_DIM), key_gain, cosine, sine_of
    )
    kv_width = k_heads * HEAD_DIM
    joined = jnp.concatenate([key_rot.reshape(tok_rows, kv_width), values], axis=1)
    initial = (
        jnp.full((k_heads, group_size, tok_rows), -jnp.inf, jnp.float32),
        jnp.zeros((k_heads, group_size, tok_rows), jnp.float32),
        jnp.zeros((k_heads, group_size, tok_rows, HEAD_DIM), jnp.float32),
    )
    final_max, denominator, summed = attend_block(
        initial, lax.all_gather(joined, "ep", axis=0, tiled=True), query_rot, kv_width
    )
    attended = (
        (summed / denominator[..., None])
        .transpose(2, 0, 1, 3)
        .reshape(tok_rows, q_heads * HEAD_DIM)
        .astype(jnp.bfloat16)
    )
    moe_tokens = moe_rows.shape[0]
    local_experts = expert_gate.shape[0]
    expert_count = local_experts * lax.axis_size("ep")
    capacity = 3 * moe_tokens * TOPK // (2 * expert_count)
    picks = moe_tokens * TOPK
    route_list = route_ids.reshape(picks)
    one_hot = (route_list[:, None] == jnp.arange(expert_count, dtype=jnp.int32)[None, :]).astype(
        jnp.int32
    )
    rank_of = jnp.sum((jnp.cumsum(one_hot, axis=0) - one_hot) * one_hot, axis=1)
    slot_of = route_list * capacity + rank_of
    owner_of = (
        jnp.full((expert_count * capacity,), moe_tokens, jnp.int32)
        .at[slot_of]
        .set(jnp.arange(picks, dtype=jnp.int32) // TOPK)
    )
    padded = jnp.concatenate([moe_rows, jnp.zeros((1, moe_rows.shape[1]), moe_rows.dtype)], axis=0)
    arrived = lax.all_to_all(
        padded[owner_of].reshape(expert_count, capacity, moe_rows.shape[1]),
        "ep",
        split_axis=0,
        concat_axis=1,
        tiled=True,
    )
    portion = lax.all_gather(arrived, "tp", axis=2, tiled=True)
    widened = portion.astype(jnp.float32)
    gate_act = jnp.einsum("erd,edf->erf", portion, expert_gate, preferred_element_type=jnp.float32)
    up_act = jnp.einsum("erd,edf->erf", portion, expert_up, preferred_element_type=jnp.float32)
    square_sum = jnp.sum(widened * widened, axis=2)
    inv_rms = lax.rsqrt(square_sum / D + 1e-06)[..., None]
    hidden = (jax.nn.silu(gate_act * inv_rms) * (up_act * inv_rms)).astype(jnp.bfloat16)
    out_cols = expert_down.shape[2]
    expert_result = jnp.einsum(
        "erf,efd->erd",
        lax.all_gather(hidden, "tp", axis=2, tiled=True),
        expert_down,
        preferred_element_type=jnp.float32,
    ).astype(jnp.bfloat16)
    returned = lax.all_to_all(expert_result, "ep", split_axis=1, concat_axis=0, tiled=True)
    flat_back = returned.reshape(expert_count * capacity, out_cols)
    picked = flat_back[slot_of].reshape(moe_tokens, TOPK, out_cols).astype(jnp.float32)
    mixing = group_weight[:, None] * expert_weight / jnp.sum(expert_weight, axis=1, keepdims=True)
    moe_out = jnp.sum(mixing[:, :, None] * picked, axis=1).astype(jnp.bfloat16)
    return (attended, moe_out)


MESH = pl.DeviceIdType.MESH


def flip(index, mask, width):
    out = 0
    bit = 1
    while bit < width:
        a, b = (index // bit) % 2, (mask // bit) % 2
        out = out + bit * (a + b - 2 * a * b)
        bit *= 2
    return out


def rope_kernel(q_ref, k_ref, v_ref, qg_ref, kg_ref, cos_ref, sin_ref, qo_ref, kv_ref):
    rows = q_ref.shape[0]
    lane = lax.broadcasted_iota(jnp.int32, (rows, 128), 1)
    one = lax.broadcasted_iota(jnp.int32, (128, 128), 0) // HEAD_DIM
    two = lax.broadcasted_iota(jnp.int32, (128, 128), 1) // HEAD_DIM
    spread = jnp.where(one == two, 1.0 / HEAD_DIM, 0.0).astype(jnp.float32)
    first = lane % 32 < 16
    low = lane < HEAD_DIM
    cosine, sine_of = cos_ref[...], sin_ref[...]

    def turned(x, gain):
        x = x.astype(jnp.float32)
        mean = jnp.dot(
            x * x, spread, preferred_element_type=jnp.float32, precision=lax.Precision.HIGHEST
        )
        y = x * lax.rsqrt(mean + 1e-06) * gain
        partner = jnp.where(first, pltpu.roll(y, 112, 1), pltpu.roll(y, 16, 1))
        return y * cosine + partner * sine_of

    q_slabs = q_ref.shape[1] // 128
    k_slabs = k_ref.shape[1] // 128
    per_kv = q_slabs // (2 * k_slabs)
    for s in range(q_slabs):
        r = turned(q_ref[:, s * 128 : (s + 1) * 128], qg_ref[...])
        r = r.astype(jnp.bfloat16).astype(jnp.float32) * HEAD_DIM ** (-0.5)
        moved = pltpu.roll(r, HEAD_DIM, 1)
        if (s // per_kv) % 2 == 0:
            pair = (jnp.where(low, r, 0.0), jnp.where(low, moved, 0.0))
        else:
            pair = (jnp.where(low, 0.0, moved), jnp.where(low, 0.0, r))
        qo_ref[2 * s] = pair[0].astype(jnp.bfloat16)
        qo_ref[2 * s + 1] = pair[1].astype(jnp.bfloat16)
    for s in range(k_slabs):
        kv_ref[s] = turned(k_ref[:, s * 128 : (s + 1) * 128], kg_ref[...]).astype(jnp.bfloat16)
        kv_ref[k_slabs + s] = v_ref[:, s * 128 : (s + 1) * 128]


def main_kernel(
    ep, picks, kv, q_ref, s0_ref, s1_ref, mix_ref, wg_hbm, wu_hbm, wd_hbm,
    att_ref, moe_ref,
    xg, hid, res, ret, kvall, wg, wu, wd,
    w_sem, d_send, d_recv, x_send, x_recv, xr_send, xr_recv,
    h_send, h_recv, hr_send, hr_recv, r_send, r_recv, k_send, k_recv,
):
    me, tme = lax.axis_index("ep"), lax.axis_index("tp")
    tx, ty = flip(tme, 1, 4), flip(tme, 2, 4)
    sides = (tx, ty)
    cap = picks.shape[1]
    half = cap // 2
    pairs = ep // 2
    width = wg.shape[1]
    chan = picks.shape[2]

    weights = [
        pltpu.make_async_copy(a, b, w_sem.at[n])
        for n, (a, b) in enumerate(((wg_hbm.at[0], wg), (wu_hbm.at[0], wu), (wd_hbm.at[0], wd)))
    ]
    for copy in weights:
        copy.start()
    barrier = pltpu.get_barrier_semaphore()
    for j in range(1, ep):
        pl.semaphore_signal(barrier, inc=1, device_id={"ep": flip(me, j, ep)}, device_id_type=MESH)
    for side in sides:
        pl.semaphore_signal(barrier, inc=1, device_id={"tp": side}, device_id_type=MESH)
    pl.semaphore_wait(barrier, ep + 1)

    def remote(src, dst, send, recv, device):
        return pltpu.make_async_remote_copy(
            src_ref=src, dst_ref=dst, send_sem=send, recv_sem=recv,
            device_id=device, device_id_type=MESH,
        )

    def dispatch(j):
        to = flip(me, j, ep)
        return remote(picks.at[to], xg.at[j, tme], d_send.at[j], d_recv.at[j], {"ep": to})

    def keys_out(j):
        return remote(kv, kvall.at[me], k_send.at[j], k_recv.at[j], {"ep": flip(me, j, ep)})

    def keys_on(j):
        block = flip(me, j - 1, ep)
        return remote(
            kvall.at[block], kvall.at[block], k_send.at[j], k_recv.at[j], {"ep": flip(me, 1, ep)}
        )

    def cross(c, n, src=None):
        src = xg.at[c, tme] if src is None else src
        return remote(src, xg.at[c, tme], x_send.at[c, n], x_recv.at[c, n], {"tp": sides[n]})

    def cross_on(c, n):
        part = xg.at[c, sides[n], pl.ds(n * half, half)]
        return remote(part, part, xr_send.at[c, n], xr_recv.at[c, n], {"tp": sides[1 - n]})

    def wide(i, n):
        return remote(
            hid.at[i, tme], hid.at[i, tme], h_send.at[i, n], h_recv.at[i, n], {"tp": sides[n]}
        )

    def wide_on(i, n):
        part = hid.at[i, sides[n], pl.ds(n * cap, cap)]
        return remote(part, part, hr_send.at[i, n], hr_recv.at[i, n], {"tp": sides[1 - n]})

    def back(i, n):
        c = 2 * i + n
        return remote(
            res.at[i, pl.ds(n * cap, cap)], ret.at[me], r_send.at[c], r_recv.at[c],
            {"ep": flip(me, c, ep)},
        )

    for j in range(1, 4):
        dispatch(j).start()
    for j in range(1, ep):
        if j == 1 or j % 2 == 0:
            keys_out(j).start()
    for j in range(4, ep):
        dispatch(j).start()

    xg[0, tme] = picks[me]
    kvall[me] = kv[...]
    for n in range(2):
        cross(0, n, picks.at[me]).start()

    def enter(c):
        dispatch(c).wait_recv()
        for n in range(2):
            cross(c, n).start()

    def relay(i):
        for d in range(2):
            for n in range(2):
                cross(2 * i + d, n).wait_recv()
                cross_on(2 * i + d, n).start()

    for c in range(1, 4):
        enter(c)
    relay(0)
    for copy in weights:
        copy.wait()

    def first_half(i):
        for d in range(2):
            for n in range(2):
                cross_on(2 * i + d, n).wait_recv()
        gate = jnp.zeros((2 * cap, width), jnp.float32)
        up = jnp.zeros((2 * cap, width), jnp.float32)
        square = jnp.zeros((2 * cap, 1), jnp.float32)
        for a in range(4):
            x = xg[pl.ds(2 * i, 2), a].reshape(2 * cap, chan)
            w = x.astype(jnp.float32)
            square = square + jnp.sum(w * w, axis=1, keepdims=True)
            gate = gate + jnp.dot(
                x, wg[a * chan : (a + 1) * chan, :], preferred_element_type=jnp.float32
            )
            up = up + jnp.dot(
                x, wu[a * chan : (a + 1) * chan, :], preferred_element_type=jnp.float32
            )
        inv = lax.rsqrt(square / D + 1e-06)
        g = gate * inv
        hid[i, tme] = (g / (1.0 + jnp.exp(-g)) * (up * inv)).astype(jnp.bfloat16)
        for n in range(2):
            wide(i, n).start()

    def second_half(i):
        for n in range(2):
            wide_on(i, n).wait_recv()
        total = jnp.zeros((2 * cap, chan), jnp.float32)
        for a in range(4):
            total = total + jnp.dot(
                hid[i, a], wd[a * width : (a + 1) * width, :], preferred_element_type=jnp.float32
            )
        res[i] = total.astype(jnp.bfloat16)

        @pl.when(i > 0)
        def _():
            back(i, 0).start()

        @pl.when(i == 0)
        def _():
            ret[me] = res[0, :cap]

        back(i, 1).start()

    heads = q_ref.shape[0]
    slabs = heads // 2
    k_slabs = kv.shape[0] // 2
    per_kv = slabs // (2 * k_slabs)
    keys_total = ep * kv.shape[1]

    def attend(m, carry):
        pp = m // (2 * per_kv)
        k = kvall[:, pp].reshape(keys_total, 128)
        v = kvall[:, k_slabs + pp].reshape(keys_total, 128)
        outs = []
        for d in range(2):
            s = lax.dot_general(
                q_ref[2 * m + d], k, (((1,), (1,)), ((), ())), preferred_element_type=jnp.float32
            )
            p = jnp.exp(s - jnp.max(s, axis=1, keepdims=True))
            den = jnp.sum(p, axis=1, keepdims=True)
            o = jnp.dot(p.astype(jnp.bfloat16), v, preferred_element_type=jnp.float32)
            outs.append(o / den)
        low = lax.broadcasted_iota(jnp.int32, outs[0].shape, 1) < HEAD_DIM
        even = jnp.where(low, outs[0], pltpu.roll(outs[1], HEAD_DIM, 1))
        odd = jnp.where(low, pltpu.roll(outs[0], HEAD_DIM, 1), outs[1])
        side = ((m // per_kv) % 2).astype(jnp.float32)
        both = jnp.where(side == 0.0, even, odd)
        att_ref[:, pl.ds(pl.multiple_of(m * 128, 128), 128)] = both.astype(jnp.bfloat16)
        return carry

    def keys_relay():
        for j in range(2, ep, 2):
            keys_out(j).wait_recv()
            keys_on(j + 1).start()

    def keys_ready():
        keys_out(1).wait_recv()
        for j in range(2, ep, 2):
            keys_on(j + 1).wait_recv()

    def step(i, carry):
        first_half(i)

        @pl.when(i < pairs - 1)
        def _():
            relay(i + 1)

        @pl.when(i == 0)
        def _():
            keys_relay()

        @pl.when(i == 1)
        def _():
            keys_ready()

        @pl.when(i < pairs - 2)
        def _():
            enter(2 * i + 4)
            enter(2 * i + 5)

        begin = slabs * jnp.maximum(i - 1, 0) * 2 // 5
        begin = jnp.where(i == pairs - 1, slabs - 1, begin)
        end = jnp.where(i == 0, 0, slabs * i * 2 // 5)
        end = jnp.where(i == pairs - 2, slabs - 1, end)
        end = jnp.where(i == pairs - 1, slabs, end)

        def hidden_on():
            for n in range(2):
                wide(i, n).wait_recv()
                wide_on(i, n).start()

        def unit(m, carried):
            attend(m, carried)
            pl.when(m == begin)(hidden_on)
            return carried

        lax.fori_loop(begin, end, unit, 0)
        pl.when(begin == end)(hidden_on)
        second_half(i)
        return carry

    lax.fori_loop(0, pairs, step, 0)

    for c in range(1, ep):
        back(c // 2, c % 2).wait_recv()
    everything = ret[...].reshape(ep * cap, chan)
    mix = mix_ref[...]
    one = jnp.dot(s0_ref[...], everything, preferred_element_type=jnp.float32)
    two = jnp.dot(s1_ref[...], everything, preferred_element_type=jnp.float32)
    moe_ref[...] = (mix[:, 0:1] * one + mix[:, 1:2] * two).astype(jnp.bfloat16)

    for c in range(ep):
        for n in range(2):
            cross(c, n).wait_send()
            cross_on(c, n).wait_send()
        if c > 0:
            dispatch(c).wait_send()
            back(c // 2, c % 2).wait_send()
            keys_out(c).wait_send()
    for i in range(pairs):
        for n in range(2):
            wide(i, n).wait_send()
            wide_on(i, n).wait_send()


def on_device(
    queries, keys, values, query_gain, key_gain, moe_rows, route_ids, group_weight,
    expert_weight, expert_gate, expert_up, expert_down,
):
    ep, tp = lax.axis_size("ep"), lax.axis_size("tp")
    moe_tokens, chan = moe_rows.shape
    cap = 3 * moe_tokens * TOPK // (2 * expert_gate.shape[0] * ep)
    fits = tp == 4 and ep == 8 and cap % 32 == 0 and expert_gate.shape[0] == 1
    if not fits or queries.shape[1] // 128 != 8 or keys.shape[1] // 128 != 2:
        return plain_on_device(
            queries, keys, values, query_gain, key_gain, moe_rows, route_ids, group_weight,
            expert_weight, expert_gate, expert_up, expert_down,
        )
    tok = queries.shape[0]
    position = lax.axis_index("ep") * tok + jnp.arange(tok, dtype=jnp.int32)
    lane = jnp.arange(128, dtype=jnp.int32)
    pair_count = HEAD_DIM // 4
    frequency = 10000.0 ** (-(lane % pair_count).astype(jnp.float32) / pair_count)
    on_rows = (lane // (2 * pair_count)) % 2 == 0
    grid_pos = jnp.where(
        on_rows[None, :], (position // GRID_W)[:, None], (position % GRID_W)[:, None]
    ).astype(jnp.float32)
    angles = grid_pos * frequency[None, :]
    sign = jnp.where((lane // pair_count) % 2 == 0, -1.0, 1.0).astype(jnp.float32)
    heads = queries.shape[1] // HEAD_DIM
    slabs = keys.shape[1] // 128
    q_turned, kv = pl.pallas_call(
        rope_kernel,
        out_shape=(
            jax.ShapeDtypeStruct((heads, tok, 128), jnp.bfloat16),
            jax.ShapeDtypeStruct((2 * slabs, tok, 128), jnp.bfloat16),
        ),
    )(
        queries, keys, values,
        jnp.tile(query_gain, 2)[None, :], jnp.tile(key_gain, 2)[None, :],
        jnp.cos(angles), jnp.sin(angles) * sign[None, :],
    )
    picks_all = moe_tokens * TOPK
    route_list = route_ids.reshape(picks_all)
    one_hot = (route_list[:, None] == jnp.arange(ep, dtype=jnp.int32)[None, :]).astype(jnp.int32)
    rank_of = jnp.sum((jnp.cumsum(one_hot, axis=0) - one_hot) * one_hot, axis=1)
    slot_of = (route_list * cap + rank_of).reshape(moe_tokens, TOPK)
    columns = jnp.arange(ep * cap, dtype=jnp.int32)[None, :]
    picked = [(slot_of[:, n : n + 1] == columns).astype(jnp.bfloat16) for n in range(TOPK)]
    sent = lax.dot_general(
        picked[0] + picked[1], moe_rows, (((0,), (0,)), ((), ())),
        preferred_element_type=jnp.float32,
    ).astype(jnp.bfloat16).reshape(ep, cap, chan)
    mixing = group_weight[:, None] * expert_weight / jnp.sum(expert_weight, axis=1, keepdims=True)
    width = expert_gate.shape[2]
    vmem = pl.BlockSpec(memory_space=pltpu.VMEM)
    hbm = pl.BlockSpec(memory_space=pl.ANY)
    dma = pltpu.SemaphoreType.DMA
    bf = jnp.bfloat16
    attended, moe_out = pl.pallas_call(
        lambda *refs: main_kernel(ep, *refs),
        out_shape=(
            jax.ShapeDtypeStruct(queries.shape, bf),
            jax.ShapeDtypeStruct(moe_rows.shape, bf),
        ),
        in_specs=[vmem] * 6 + [hbm] * 3,
        out_specs=(vmem, vmem),
        scratch_shapes=[
            pltpu.VMEM((ep, tp, cap, chan), bf),
            pltpu.VMEM((ep // 2, tp, 2 * cap, width), bf),
            pltpu.VMEM((ep // 2, 2 * cap, chan), bf),
            pltpu.VMEM((ep, cap, chan), bf),
            pltpu.VMEM((ep, 2 * slabs, tok, 128), bf),
            pltpu.VMEM(expert_gate.shape[1:], bf),
            pltpu.VMEM(expert_up.shape[1:], bf),
            pltpu.VMEM(expert_down.shape[1:], bf),
            dma((3,)), dma((ep,)), dma((ep,)),
            dma((ep, 2)), dma((ep, 2)), dma((ep, 2)), dma((ep, 2)),
            dma((ep // 2, 2)), dma((ep // 2, 2)), dma((ep // 2, 2)), dma((ep // 2, 2)),
            dma((ep,)), dma((ep,)), dma((ep,)), dma((ep,)),
        ],
        compiler_params=pltpu.CompilerParams(
            collective_id=0, has_side_effects=True, vmem_limit_bytes=60 * 1024 * 1024
        ),
    )(sent, kv, q_turned, picked[0], picked[1], mixing, expert_gate, expert_up, expert_down)
    return (attended, moe_out)


def solution(mesh):
    placed = (
        P("ep", "tp"),
        P("ep", "tp"),
        P("ep", "tp"),
        P(),
        P(),
        P("ep", "tp"),
        P("ep", None),
        P("ep"),
        P("ep", None),
        P("ep", None, "tp"),
        P("ep", None, "tp"),
        P("ep", None, "tp"),
    )
    return jax.shard_map(
        on_device,
        mesh=mesh,
        in_specs=placed,
        out_specs=(P("ep", "tp"), P("ep", "tp")),
        check_vma=False,
    )
```
